32 devices in a mesh: ep: 8 (over z, x), tp: 4 (over y, core).
Axes of the slice: x: 2, y: 2, z: 4, core: 2. Of those that a mesh axis runs over, the one named last changes fastest.
Arguments:
- tokens: bfloat16 [192, 3072], P('ep'), may hold values from -6 to 6
- norm_gain: float32 [3072], replicated, may hold values from 0.1 to 1.9
- routing: int32 [192, 4], P('ep'), may hold values from 0 to 7, all different within a row; in each aligned block of 24 rows (0 to 23, 24 to 47, ...) at most 13 rows name the same one
- route_weight: float32 [192, 4], P('ep'), may hold values from 0.05 to 1
- w_gate: bfloat16 [8, 3072, 3072], P('ep', None, 'tp'), may hold values from -0.3125 to 0.3125
- w_up: bfloat16 [8, 3072, 3072], P('ep', None, 'tp'), may hold values from -0.3125 to 0.3125
- w_down: bfloat16 [8, 3072, 3072], P('ep', 'tp'), may hold values from -0.01953125 to 0.01953125
Outputs:
- mixed: bfloat16 [192, 3072], P('ep', 'tp')
The draws below stay inside these ranges and needn't reach their ends.
Inputs may be any that keep to these rules, and one draw needn't show every extreme that they name: `routing`: each row names 4 different experts. Within the rows of one device (aligned blocks of 24 rows) no expert is named by more than 13 rows, a bound that some block reaches.
All inputs are finite; a program needn't handle non-finite values.
Results may differ from the reference program's by a relative error of at most 0.019.
Values may be sent and summed in bfloat16 or wider, within the bound.
No kernel may reach another device: no remote copies, remote signals or barrier semaphores. Data moves between devices by JAX's collectives and lax.ppermute only.
A program may use at most 64 MiB of HBM per device.

```python
import math
import jax
import jax.numpy as jnp
import numpy as np
from jax import lax

D = 3072
FF = 3072
TOP_K = 4
TOK_DEV = 24
EXPERTS = 8
CAP = 13
TOKENS = 192
N_EP = 8
N_TP = 4


def strengthened(result, own_key, source, target, parts, factor):
    owner, partner = [(jnp.arange(result.shape[dim]) // (result.shape[dim] // parts)).reshape([-1 if axis == dim else 1 for axis in range(result.ndim)]) for dim in (source, target)]
    chosen = jax.random.permutation(own_key, parts)[partner]
    strong = (owner == chosen) | (owner == (partner + parts // 2) % parts)
    return jnp.where(strong, factor * result, result)


def level_of(key, extent, split, smallest, high):
    loudness, own = 1.0, jax.random.fold_in(key, 6)
    for axis_at, parts in split:
        draws = jnp.exp(jax.random.uniform(jax.random.fold_in(own, axis_at), (parts,), jnp.float32, smallest / len(split), high / len(split)))
        loudness = loudness * jnp.repeat(draws, extent[axis_at] // parts).reshape([-1 if axis == axis_at else 1 for axis in range(len(extent))])
    return loudness


def routed_block(own_key, own, number, rows, count, top, limit, slope):
    sequence = jax.random.permutation(own_key, count)
    crowded, ordinary = load_shares(count, rows * top, limit, slope, True), load_shares(count, rows * top, limit, slope, False)
    places = jnp.arange(count)

    def named(sizes, turn):
        used = int((sizes > 0).sum())
        fixed = max(1, used // 4)
        passed = fixed + (places - fixed + turn * (used - fixed)) % max(1, count - fixed)
        return jnp.zeros((count,), jnp.int32).at[sequence[jnp.where(places < fixed, places, passed)]].set(jnp.asarray(sizes, jnp.int32))

    sizes = jnp.where(number % 4 == 0, named(crowded, number // 4), named(ordinary, number - number // 4 - 1))
    mixed = jax.random.permutation(jax.random.fold_in(own, 3), count)
    giver, taker = mixed[0:count // 2 * 2:2], mixed[1:count // 2 * 2:2]
    room = jnp.minimum(sizes[giver] - 1, limit - sizes[taker]) // 2
    room = jnp.where((giver == sequence[0]) | (taker == sequence[0]) | (sizes[taker] == 0), 0, jnp.maximum(room, 0))
    passed = jax.random.randint(jax.random.fold_in(own, 4), (count // 2,), 0, 1 << 20) % (room + 1)
    sizes = sizes.at[giver].add(-passed).at[taker].add(passed)
    labels = jnp.searchsorted(jnp.cumsum(sizes), jnp.arange(rows * top), side="right").astype(jnp.int32)
    grid = labels.reshape(top, rows).T
    grid = grid[jax.random.permutation(jax.random.fold_in(own, 1), rows)]
    turn = jax.random.randint(jax.random.fold_in(own, 2), (rows, 1), 0, top)
    return jnp.take_along_axis(grid, (jnp.arange(top)[None, :] + turn) % top, axis=1)


def load_shares(count, total, reach, lean, full):
    portions = [(1 << 20) // math.isqrt(grade ** lean) + 1 for grade in range(1, count + 1)]
    largest = reach if full else min(reach, max(-(-total // count), total * portions[0] // sum(portions)))
    least = 1 if total - largest >= count - 1 else 0
    counts, surplus = [largest] + [least] * (count - 1), total - largest - least * (count - 1)
    while surplus > 0:
        movable = [i for i in range(1, count) if counts[i] < largest] or [i for i in range(1, count) if counts[i] < reach]
        mass, budget = sum([portions[i] for i in movable]), surplus
        for i in movable:
            addition = min(reach - counts[i], max(1, budget * portions[i] // mass), surplus)
            counts[i] = counts[i] + addition
            surplus = surplus - addition
    return np.array(counts)


def scatter_about(own_key, shape, width, limit, split=(), kind=jnp.bfloat16):
    drawn = jax.random.normal(own_key, shape, jnp.float32) * width
    if len(split) > 0:
        drawn = level_of(own_key, shape, split, -0.22, 0.18) * drawn
    return jnp.clip(drawn, min=-limit, max=limit).astype(kind)


def bell_draw_with(rng, dims, deviation, limit, pieces, heavy, kind=jnp.bfloat16):
    entries = deviation * jax.random.normal(rng, dims, jnp.float32)
    if pieces:
        entries = entries * level_of(rng, dims, pieces, -0.22, 0.18)
    return jnp.clip(strengthened(entries, jax.random.fold_in(rng, 3), *heavy), -limit, limit).astype(kind)


def setup_inputs(seed: int = 0) -> dict:
    streams_of = jax.random.split(jax.random.key(seed), 8)
    tokens = scatter_about(streams_of[0], (TOKENS, D), 1.0, 6.0, ((0, 8),))
    norm_gain = jnp.clip(1.0 + 0.18 * jax.random.normal(streams_of[1], (D,), jnp.float32), 0.1, 1.9)
    routing_keys = jax.random.split(jax.random.fold_in(streams_of[2], 1), TOKENS // TOK_DEV)
    routing_turns = jax.random.permutation(jax.random.fold_in(streams_of[2], 3), TOKENS // TOK_DEV)
    routing = jax.vmap(lambda own, number: routed_block(jax.random.fold_in(streams_of[2], 2), own, number, TOK_DEV, EXPERTS, TOP_K, CAP, 2))(routing_keys, routing_turns).reshape((TOKENS, TOP_K))
    route_weight = jnp.clip(jnp.exp(math.log(1.0) - 2.9957323 * jax.random.uniform(streams_of[3], (TOKENS, TOP_K), jnp.float32) ** level_of(streams_of[3], (TOKENS, TOP_K), ((0, 8),), -0.2, 0.2)), 0.05, 1.0)
    w_gate = scatter_about(streams_of[4], (EXPERTS, D, FF), (D // 9) ** -0.5, 0.3125, ((0, 8), (2, 4)))
    w_up = scatter_about(streams_of[5], (EXPERTS, D, FF), (D // 9) ** -0.5, 0.3125, ((0, 8), (2, 4)))
    w_down = bell_draw_with(streams_of[6], (EXPERTS, FF, D), (64 * FF) ** -0.5, 0.01953125, ((0, 8), (1, 4)), (1, 2, 4, 2.0))
    return {"tokens": tokens, "norm_gain": norm_gain, "routing": routing, "route_weight": route_weight, "w_gate": w_gate, "w_up": w_up, "w_down": w_down}


NORM_EPS = 1e-06
CLAMP_LIMIT = 7.0
SIGMOID_SCALE = 1.702

def slot_index(route_rows, expert_total, capacity):
    flat_ids = route_rows.reshape(-1)
    one_hot = (flat_ids[:, None] == jnp.arange(expert_total, dtype=jnp.int32)[None, :]).astype(jnp.int32)
    before = jnp.cumsum(one_hot, axis=0) - one_hot
    ranked = lax.optimization_barrier(jnp.sum(before * one_hot, axis=1))
    return (flat_ids * capacity + ranked).astype(jnp.int32)

def normed(tokens, norm_gain):
    values = tokens.astype(jnp.float32)
    scaled = values * lax.rsqrt(lax.optimization_barrier(jnp.mean(values * values, axis=-1, keepdims=True)) + NORM_EPS)
    return (scaled * norm_gain).astype(jnp.bfloat16)

def clamped_unit(gate_pre, up_pre):
    gated = jnp.minimum(gate_pre, CLAMP_LIMIT)
    upper = jnp.clip(up_pre, -CLAMP_LIMIT, CLAMP_LIMIT)
    return ((upper + 1.0) * gated * jax.nn.sigmoid(SIGMOID_SCALE * gated)).astype(jnp.bfloat16)

def reference(tokens, norm_gain, routing, route_weight, w_gate, w_up, w_down):
    normal = normed(tokens, norm_gain)
    dest = jax.vmap(lambda block_routes: slot_index(block_routes, EXPERTS, CAP))(routing.reshape(N_EP, TOK_DEV, TOP_K))
    slot_ids = jnp.arange(EXPERTS * CAP, dtype=jnp.int32)
    select = lax.optimization_barrier(jnp.sum(dest.reshape(N_EP, 1, TOK_DEV, TOP_K) == slot_ids[None, :, None, None], axis=3))
    sending = jnp.einsum('bst,btd->bsd', select.astype(jnp.float32), normal.reshape(N_EP, TOK_DEV, D).astype(jnp.float32)).astype(jnp.bfloat16)
    inbox = sending.reshape(N_EP, EXPERTS, CAP, D).transpose(1, 0, 2, 3).reshape(EXPERTS, N_EP * CAP, D)

    def expert(operands):
        rows_in, gate_mat, up_mat, down_mat = operands
        gate_pre = jnp.dot(rows_in, gate_mat, preferred_element_type=jnp.float32)
        up_pre = jnp.dot(rows_in, up_mat, preferred_element_type=jnp.float32)
        hidden = clamped_unit(gate_pre, up_pre)
        row_total = hidden.shape[0]
        partial_value = jnp.einsum('rjf,jfd->jrd', hidden.reshape(row_total, N_TP, FF // N_TP).astype(jnp.float32), down_mat.reshape(N_TP, FF // N_TP, D).astype(jnp.float32))
        rounded = lax.optimization_barrier(partial_value.astype(jnp.bfloat16))
        return lax.optimization_barrier(jnp.sum(rounded.astype(jnp.float32), axis=0)).astype(jnp.bfloat16)
    outbox = lax.map(expert, (inbox, w_gate, w_up, w_down))
    back = outbox.reshape(EXPERTS, N_EP, CAP, D).transpose(1, 0, 2, 3).reshape(N_EP, EXPERTS * CAP, D)
    picked = jnp.take_along_axis(back, dest[:, :, None], axis=1).reshape(TOKENS, TOP_K, D)
    mixed = lax.optimization_barrier(jnp.sum(picked.astype(jnp.float32) * route_weight[:, :, None], axis=1))
    return mixed.astype(jnp.bfloat16)
```

```python
import functools

import jax
import jax.numpy as jnp
from jax import lax
from jax.experimental import pallas as pl
from jax.experimental.pallas import tpu as pltpu
from jax.sharding import Mesh, PartitionSpec as P

NORM_EPS = 1e-06
CLAMP_LIMIT = 7.0
SIGMOID_SCALE = 1.702
CORES = 2
TILE_ROWS = 16
LANES = 128

VMEM = pl.BlockSpec(memory_space=pltpu.VMEM)
SMEM = pl.BlockSpec(memory_space=pltpu.SMEM)


def dot(a, b):
    return jnp.dot(a, b, preferred_element_type=jnp.float32)


def slot_select(routes, slots, pad, tok_count):
    top_count = routes.shape[0]
    row = lax.broadcasted_iota(jnp.int32, (slots, tok_count), 0)
    expert = row // pad
    place = row - expert * pad
    named = [routes[k][None, :] == expert for k in range(top_count)]
    chosen = functools.reduce(jnp.logical_or, named)
    earlier = lax.broadcasted_iota(jnp.int32, (tok_count, tok_count), 0) < lax.broadcasted_iota(
        jnp.int32, (tok_count, tok_count), 1
    )
    rank = dot(chosen.astype(jnp.bfloat16), earlier.astype(jnp.bfloat16))
    here = chosen & (rank == place.astype(jnp.float32))
    return named, here


def gather_kernel(core_ref, tok_ref, gain_ref, route_ref, out_ref, *, pad):
    tok_count = tok_ref.shape[0]
    half = out_ref.shape[1]
    values = tok_ref[...].astype(jnp.float32)
    scale = lax.rsqrt(jnp.mean(values * values, axis=-1, keepdims=True) + NORM_EPS)
    lanes = pl.ds(pl.multiple_of(core_ref[0] * half, half), half)
    own = tok_ref[:, lanes].astype(jnp.float32)
    normal = (own * scale * gain_ref[:, lanes]).astype(jnp.bfloat16)
    _, here = slot_select(route_ref[...], out_ref.shape[0], pad, tok_count)
    out_ref[...] = dot(here.astype(jnp.bfloat16), normal).astype(jnp.bfloat16)


def first_kernel(core_ref, x_ref, gate_ref, up_ref, gate_out, up_out):
    half = x_ref.shape[1]
    rows = pl.ds(pl.multiple_of(core_ref[0] * half, half), half)
    gate_out[...] = dot(x_ref[...], gate_ref[0, rows, :])
    up_out[...] = dot(x_ref[...], up_ref[0, rows, :])


def column_block(down_ref, group, core, width):
    if width % LANES == 0:
        start = (group * CORES + core) * width
        return down_ref[0, :, pl.ds(pl.multiple_of(start, width), width)]
    first, second = [
        down_ref[0, :, (group * CORES + i) * width : (group * CORES + i + 1) * width]
        for i in range(CORES)
    ]
    return jnp.where(core == 0, first, second)


def second_kernel(
    core_ref, x_ref, gate_in, up_in, gate_ref, up_ref, down_ref, hidden_ref, away_ref
):
    half = x_ref.shape[1]
    other = (CORES - 1) - core_ref[0]
    rows = pl.ds(pl.multiple_of(other * half, half), half)
    gate_pre = gate_in[...] + dot(x_ref[...], gate_ref[0, rows, :])
    up_pre = up_in[...] + dot(x_ref[...], up_ref[0, rows, :])
    gated = jnp.minimum(gate_pre, CLAMP_LIMIT)
    upper = jnp.clip(up_pre, -CLAMP_LIMIT, CLAMP_LIMIT)
    hidden = ((upper + 1.0) * gated * jax.nn.sigmoid(SIGMOID_SCALE * gated)).astype(jnp.bfloat16)
    hidden_ref[...] = hidden
    groups, _, width = away_ref.shape
    for group in range(groups):
        block = column_block(down_ref, group, other, width)
        away_ref[group] = dot(hidden, block).astype(jnp.bfloat16)


def third_kernel(core_ref, hidden_ref, down_ref, own_ref):
    groups, _, width = own_ref.shape
    for group in range(groups):
        block = column_block(down_ref, group, core_ref[0], width)
        own_ref[group] = dot(hidden_ref[...], block)


def add_kernel(own_ref, away_ref, out_ref, *, blocks, pad):
    groups, _, width = own_ref.shape
    for group in range(groups):
        total = own_ref[group] + away_ref[group].astype(jnp.float32)
        out_ref[:, group] = total.astype(jnp.bfloat16).reshape(blocks, pad, width)


def combine_kernel(back_ref, route_ref, weight_ref, out_ref, *, pad):
    experts, groups, _, width = back_ref.shape
    tok_count = out_ref.shape[0]
    slots = experts * pad
    named, here = slot_select(route_ref[...], slots, pad, tok_count)
    mix = jnp.zeros((slots, tok_count), jnp.float32)
    for k, at in enumerate(named):
        mix = jnp.where(at & here, weight_ref[k][None, :], mix)
    high = mix.astype(jnp.bfloat16)
    low = (mix - high.astype(jnp.float32)).astype(jnp.bfloat16)
    total = jnp.zeros((tok_count, width), jnp.float32)
    for group in range(groups):
        rows = back_ref[:, group].reshape(slots, width)
        for part in (high, low):
            total += lax.dot_general(
                part, rows, (((0,), (0,)), ((), ())), preferred_element_type=jnp.float32
            )
    out_ref[...] = total.astype(jnp.bfloat16)


def call(kernel, out_shape, args, limit, flops, moved):
    specs = [SMEM if a.dtype == jnp.int32 and a.ndim == 1 else VMEM for a in args]
    return pl.pallas_call(
        kernel,
        out_shape=out_shape,
        in_specs=specs,
        out_specs=jax.tree.map(lambda _: VMEM, out_shape),
        compiler_params=pltpu.CompilerParams(vmem_limit_bytes=limit),
        cost_estimate=pl.CostEstimate(flops=flops, bytes_accessed=moved, transcendentals=0),
    )(*args)


def local(tokens, norm_gain, routing, route_weight, w_gate, w_up, w_down):
    tok_count, width = tokens.shape
    top_count = routing.shape[1]
    blocks = lax.axis_size("ep")
    groups = lax.axis_size("y")
    experts = blocks * w_gate.shape[0]
    hidden_width = w_gate.shape[2]
    capacity = max(2, tok_count * top_count // experts + 1)
    pad = -(-capacity // TILE_ROWS) * TILE_ROWS
    rows = blocks * pad
    half = width // CORES
    share = width // (groups * CORES)
    core = lax.axis_index("core").reshape(1)
    swap = [(i, CORES - 1 - i) for i in range(CORES)]
    routes = routing.T
    weights = route_weight.T
    bf16, f32 = jnp.bfloat16, jnp.float32
    mib = 1 << 20

    sending = call(
        functools.partial(gather_kernel, pad=pad),
        jax.ShapeDtypeStruct((experts * pad, half), bf16),
        (core, tokens, norm_gain.reshape(1, width), routes),
        16 * mib,
        20 * 10**9,
        60 * 10**6,
    )
    own = lax.all_to_all(
        sending.reshape(blocks, pad, half), "ep", split_axis=0, concat_axis=0, tiled=True
    ).reshape(rows, half)
    peer = lax.ppermute(own, "core", swap)
    gate = w_gate
    up = w_up
    down = w_down
    pre = jax.ShapeDtypeStruct((rows, hidden_width), f32)
    step = 2 * rows * half * hidden_width
    gate_part, up_part = call(
        first_kernel, (pre, pre), (core, own, gate, up), 16 * mib, 2 * step, 4 * half * hidden_width
    )
    hidden, away = call(
        second_kernel,
        (
            jax.ShapeDtypeStruct((rows, hidden_width), bf16),
            jax.ShapeDtypeStruct((groups, rows, share), bf16),
        ),
        (core, peer, gate_part, up_part, gate, up, down),
        16 * mib,
        3 * step,
        6 * half * hidden_width,
    )
    arrived = lax.ppermute(away, "core", swap)
    kept = call(
        third_kernel,
        jax.ShapeDtypeStruct((groups, rows, share), f32),
        (core, hidden, down),
        16 * mib,
        step,
        2 * half * hidden_width,
    )
    summed = call(
        functools.partial(add_kernel, blocks=blocks, pad=pad),
        jax.ShapeDtypeStruct((blocks, groups, pad, share), bf16),
        (kept, arrived),
        16 * mib,
        rows * half,
        8 * rows * half,
    )
    back = lax.all_to_all(
        summed.reshape(blocks * groups, pad, share),
        ("ep", "y"),
        split_axis=0,
        concat_axis=0,
        tiled=True,
    ).reshape(blocks, groups, pad, share)
    return call(
        functools.partial(combine_kernel, pad=pad),
        jax.ShapeDtypeStruct((tok_count, share), bf16),
        (back, routes, weights),
        16 * mib,
        4 * rows * tok_count * half,
        4 * rows * half,
    )


def solution(mesh):
    blocks, shares = mesh.devices.shape
    split = Mesh(mesh.devices.reshape(blocks, shares // CORES, CORES), ("ep", "y", "core"))
    tp = ("y", "core")
    placed = (
        P("ep", None),
        P(),
        P("ep", None),
        P("ep", None),
        P("ep", None, tp),
        P("ep", None, tp),
        P("ep", tp, None),
    )
    return jax.shard_map(
        local, mesh=split, in_specs=placed, out_specs=P("ep", tp), check_vma=False
    )
```

```python
import functools

import jax
import jax.numpy as jnp
from jax import lax
from jax.experimental import pallas as pl
from jax.experimental.pallas import tpu as pltpu
from jax.sharding import Mesh, PartitionSpec as P

NORM_EPS = 1e-06
CLAMP_LIMIT = 7.0
SIGMOID_SCALE = 1.702
CORES = 2
TILE_ROWS = 16
LANES = 128
MIB = 1 << 20

VMEM = pl.BlockSpec(memory_space=pltpu.VMEM)
SMEM = pl.BlockSpec(memory_space=pltpu.SMEM)
HBM = pl.BlockSpec(memory_space=pltpu.HBM)


def round_up(count, unit):
    return -(-count // unit) * unit


class Wire:
    def __init__(self, messages, capacity, width):
        self.messages = messages
        self.capacity = capacity
        self.pad = round_up(capacity, TILE_ROWS)
        self.lanes = LANES if width % LANES == 0 else width
        self.columns = width // self.lanes
        self.stride = round_up(self.columns * capacity, TILE_ROWS)
        self.rows = messages * self.stride

    def window(self, message, column):
        start = message * self.stride + column * self.capacity
        return slice(start, start + self.pad)

    def block(self, column):
        return slice(column * self.lanes, (column + 1) * self.lanes)

    def scratch(self):
        return pltpu.VMEM((self.rows + self.pad, self.lanes), jnp.float32)

    def pack(self, scratch, out_ref, get):
        blank = jnp.zeros((TILE_ROWS, self.lanes), jnp.float32)
        for message in range(self.messages):
            end = (message + 1) * self.stride
            scratch[end - TILE_ROWS : end, :] = blank
            for column in range(self.columns):
                scratch[self.window(message, column), :] = get(message, column)
        out_ref[...] = scratch[: self.rows, :].astype(jnp.bfloat16)

    def unpack(self, wire_ref, scratch, put):
        scratch[: self.rows, :] = wire_ref[...].astype(jnp.float32)
        scratch[self.rows :, :] = jnp.zeros((self.pad, self.lanes), jnp.float32)
        for message in range(self.messages):
            for column in range(self.columns):
                put(message, column, scratch[self.window(message, column), :].astype(jnp.bfloat16))


def dot(a, b):
    return jnp.dot(a, b, preferred_element_type=jnp.float32)


def gather_kernel(
    core_ref, tok_hbm, gain_hbm, route_hbm, out_ref, tok_ref, gain_ref, route_ref, scratch, sems, *, wire
):
    tok_count, width = tok_ref.shape
    half = width // CORES
    copies = [
        pltpu.make_async_copy(source, target, sems.at[i])
        for i, (source, target) in enumerate(
            ((route_hbm, route_ref), (tok_hbm, tok_ref), (gain_hbm, gain_ref))
        )
    ]
    for copy in copies:
        copy.start()
    copies[0].wait()
    slots = wire.messages * wire.pad
    row = lax.broadcasted_iota(jnp.int32, (slots, tok_count), 0)
    expert = row // wire.pad
    place = (row - expert * wire.pad).astype(jnp.float32)
    chosen = functools.reduce(
        jnp.logical_or, [route_ref[k][None, :] == expert for k in range(route_ref.shape[0])]
    )
    earlier = lax.broadcasted_iota(jnp.int32, (tok_count, tok_count), 0) < lax.broadcasted_iota(
        jnp.int32, (tok_count, tok_count), 1
    )
    rank = dot(chosen.astype(jnp.bfloat16), earlier.astype(jnp.bfloat16))
    select = (chosen & (rank == place)).astype(jnp.bfloat16)
    copies[1].wait()
    values = tok_ref[...].astype(jnp.float32)
    scale = lax.rsqrt(jnp.mean(values * values, axis=-1, keepdims=True) + NORM_EPS)
    copies[2].wait()
    lanes = pl.ds(pl.multiple_of(core_ref[0] * half, half), half)
    own = tok_ref[:, lanes].astype(jnp.float32)
    normal = (own * scale * gain_ref[:, lanes]).astype(jnp.bfloat16)
    rows = dot(select, normal)
    wire.pack(
        scratch,
        out_ref,
        lambda message, column: rows[
            message * wire.pad : (message + 1) * wire.pad, wire.block(column)
        ],
    )


def unpack_rows(wire, wire_ref, scratch, x_ref):
    def put(message, column, rows):
        x_ref[message * wire.pad : (message + 1) * wire.pad, wire.block(column)] = rows

    wire.unpack(wire_ref, scratch, put)


def first_kernel(
    core_ref, wire_ref, gate_ref, up_ref, _, gate_out, up_out, scratch, x_ref, *, wire
):
    unpack_rows(wire, wire_ref, scratch, x_ref)
    half = x_ref.shape[1]
    rows = pl.ds(pl.multiple_of(core_ref[0] * half, half), half)
    gate_out[...] = dot(x_ref[...], gate_ref[0, rows, :])
    up_out[...] = dot(x_ref[...], up_ref[0, rows, :])


def column_block(down_ref, group, core, width):
    if width % LANES == 0:
        start = (group * CORES + core) * width
        return down_ref[0, :, pl.ds(pl.multiple_of(start, width), width)]
    first, second = [
        down_ref[0, :, (group * CORES + i) * width : (group * CORES + i + 1) * width]
        for i in range(CORES)
    ]
    return jnp.where(core == 0, first, second)


def second_kernel(
    core_ref,
    wire_ref,
    gate_in,
    up_in,
    gate_ref,
    up_ref,
    down_ref,
    hidden_ref,
    away_ref,
    scratch,
    x_ref,
    *,
    wire,
):
    unpack_rows(wire, wire_ref, scratch, x_ref)
    half = x_ref.shape[1]
    other = (CORES - 1) - core_ref[0]
    rows = pl.ds(pl.multiple_of(other * half, half), half)
    gate_pre = gate_in[...] + dot(x_ref[...], gate_ref[0, rows, :])
    up_pre = up_in[...] + dot(x_ref[...], up_ref[0, rows, :])
    gated = jnp.minimum(gate_pre, CLAMP_LIMIT)
    upper = jnp.clip(up_pre, -CLAMP_LIMIT, CLAMP_LIMIT)
    hidden = ((upper + 1.0) * gated * jax.nn.sigmoid(SIGMOID_SCALE * gated)).astype(jnp.bfloat16)
    hidden_ref[...] = hidden
    groups, _, width = away_ref.shape
    for group in range(groups):
        block = column_block(down_ref, group, other, width)
        away_ref[group] = dot(hidden, block).astype(jnp.bfloat16)


def turned(eye, table):
    return lax.dot_general(
        eye, table, (((1,), (1,)), ((), ())), preferred_element_type=jnp.float32
    )


def third_kernel(
    core_ref, hidden_ref, down_ref, route_ref, weight_ref, own_ref, mix_ref, *, wire, experts
):
    groups, _, width = own_ref.shape
    for group in range(groups):
        block = column_block(down_ref, group, core_ref[0], width)
        own_ref[group] = dot(hidden_ref[...], block)

    bf16, f32 = jnp.bfloat16, jnp.float32
    top_count, tok_count = route_ref.shape
    square = (tok_count, tok_count)
    down_at = lax.broadcasted_iota(jnp.int32, square, 0)
    across = lax.broadcasted_iota(jnp.int32, square, 1)
    eye = (down_at == across).astype(bf16)
    routes = turned(eye, route_ref[...].astype(bf16)).astype(jnp.int32)
    weights = weight_ref[...]
    high = weights.astype(bf16)
    low = (weights - high.astype(f32)).astype(bf16)
    weights = turned(eye, high) + turned(eye, low)
    lane = lax.broadcasted_iota(jnp.int32, (1, wire.rows), 1)
    message = lane // wire.stride
    offset = (lane - message * wire.stride).astype(f32)
    expert = message // groups
    weight = jnp.zeros((tok_count, wire.rows), f32)
    chosen = jnp.zeros((tok_count, wire.rows), f32)
    for k in range(top_count):
        at = routes[:, k : k + 1] == expert
        weight = jnp.where(at, weights[:, k : k + 1], weight)
        chosen = jnp.where(at, 1.0, chosen)
    rank = dot((across < down_at).astype(bf16), chosen.astype(bf16))
    away = offset - rank
    mix = jnp.concatenate(
        [
            jnp.where(away == float(column * wire.capacity), weight, 0.0)
            for column in range(wire.columns)
        ],
        axis=0,
    )
    high = mix.astype(bf16)
    mix_ref[0] = high
    mix_ref[1] = (mix - high.astype(f32)).astype(bf16)


def add_kernel(own_ref, away_ref, out_ref, scratch, *, wire):
    groups = own_ref.shape[0]

    def get(message, column):
        block, group = divmod(message, groups)
        rows = slice(block * wire.pad, (block + 1) * wire.pad)
        lanes = wire.block(column)
        return own_ref[group, rows, lanes] + away_ref[group, rows, lanes].astype(jnp.float32)

    wire.pack(scratch, out_ref, get)


def combine_kernel(back_ref, mix_ref, out_ref, *, wire):
    tok_count = out_ref.shape[0]
    total = dot(mix_ref[0], back_ref[...]) + dot(mix_ref[1], back_ref[...])
    for column in range(wire.columns):
        rows = total[column * tok_count : (column + 1) * tok_count]
        out_ref[:, wire.block(column)] = rows.astype(jnp.bfloat16)


def in_hbm(array):
    return pltpu.with_memory_space_constraint(array, pltpu.HBM)


def call(kernel, out_shape, args, flops, moved, scratch=(), spaces=None, limit=16 * MIB):
    specs = spaces or [SMEM if a.dtype == jnp.int32 and a.ndim == 1 else VMEM for a in args]
    return pl.pallas_call(
        kernel,
        out_shape=out_shape,
        in_specs=specs,
        out_specs=jax.tree.map(lambda _: VMEM, out_shape),
        scratch_shapes=scratch,
        compiler_params=pltpu.CompilerParams(vmem_limit_bytes=limit),
        cost_estimate=pl.CostEstimate(flops=flops, bytes_accessed=moved, transcendentals=0),
    )(*args)


def local(tokens, norm_gain, routing, route_weight, w_gate, w_up, w_down):
    tok_count, width = tokens.shape
    top_count = routing.shape[1]
    blocks = lax.axis_size("ep")
    groups = lax.axis_size("y")
    experts = blocks * w_gate.shape[0]
    hidden_width = w_gate.shape[2]
    capacity = max(2, tok_count * top_count // experts + 1)
    half = width // CORES
    share = width // (groups * CORES)
    there = Wire(blocks, capacity, half)
    home = Wire(blocks * groups, capacity, share)
    rows = blocks * there.pad
    core = lax.axis_index("core").reshape(1)
    swap = [(i, CORES - 1 - i) for i in range(CORES)]
    routes = routing.T
    weights = route_weight.T
    bf16, f32 = jnp.bfloat16, jnp.float32
    shape = jax.ShapeDtypeStruct

    sending = call(
        functools.partial(gather_kernel, wire=there),
        shape((there.rows, there.lanes), bf16),
        (core, *[in_hbm(a) for a in (tokens, norm_gain.reshape(1, width), routes)]),
        40 * 10**9,
        60 * 10**6,
        scratch=(
            pltpu.VMEM((tok_count, width), bf16),
            pltpu.VMEM((1, width), f32),
            pltpu.VMEM((top_count, tok_count), jnp.int32),
            there.scratch(),
            pltpu.SemaphoreType.DMA((3,)),
        ),
        spaces=[SMEM, HBM, HBM, HBM],
    )
    own = lax.all_to_all(
        sending.reshape(blocks, there.stride, there.lanes),
        "ep",
        split_axis=0,
        concat_axis=0,
        tiled=True,
    ).reshape(there.rows, there.lanes)
    peer = lax.ppermute(own, "core", swap)
    pre = shape((rows, hidden_width), f32)
    step = 2 * rows * half * hidden_width
    unpacking = (there.scratch(), pltpu.VMEM((rows, half), bf16))
    gate_part, up_part = call(
        functools.partial(first_kernel, wire=there),
        (pre, pre),
        (core, own, w_gate, w_up, w_down),
        2 * step,
        4 * half * hidden_width,
        scratch=unpacking,
    )
    hidden, away = call(
        functools.partial(second_kernel, wire=there),
        (shape((rows, hidden_width), bf16), shape((groups, rows, share), bf16)),
        (core, peer, gate_part, up_part, w_gate, w_up, w_down),
        3 * step,
        6 * half * hidden_width,
        scratch=unpacking,
    )
    arrived = lax.ppermute(away, "core", swap)
    kept, mix = call(
        functools.partial(third_kernel, wire=home, experts=experts),
        (
            shape((groups, rows, share), f32),
            shape((2, home.columns * tok_count, home.rows), bf16),
        ),
        (core, hidden, w_down, routes, weights),
        step,
        2 * half * hidden_width,
    )
    summed = call(
        functools.partial(add_kernel, wire=home),
        shape((home.rows, home.lanes), bf16),
        (kept, arrived),
        rows * half,
        8 * rows * half,
        scratch=(home.scratch(),),
    )
    back = lax.all_to_all(
        summed.reshape(blocks * groups, home.stride, home.lanes),
        ("ep", "y"),
        split_axis=0,
        concat_axis=0,
        tiled=True,
    ).reshape(home.rows, home.lanes)
    return call(
        functools.partial(combine_kernel, wire=home),
        shape((tok_count, share), bf16),
        (back, mix),
        4 * rows * tok_count * half,
        4 * rows * half,
    )


def solution(mesh):
    blocks, shares = mesh.devices.shape
    split = Mesh(mesh.devices.reshape(blocks, shares // CORES, CORES), ("ep", "y", "core"))
    tp = ("y", "core")
    placed = (
        P("ep", None),
        P(),
        P("ep", None),
        P("ep", None),
        P("ep", None, tp),
        P("ep", None, tp),
        P("ep", tp, None),
    )
    return jax.shard_map(
        local, mesh=split, in_specs=placed, out_specs=P("ep", tp), check_vma=False
    )
```

```python
import functools

import jax
import jax.numpy as jnp
from jax import lax
from jax.experimental import pallas as pl
from jax.experimental.pallas import tpu as pltpu
from jax.sharding import Mesh, PartitionSpec as P

NORM_EPS = 1e-06
CLAMP_LIMIT = 7.0
SIGMOID_SCALE = 1.702
CORES = 2
MOST_EXCHANGES = 16
TILE_ROWS = 16
LANES = 128
MIB = 1 << 20

VMEM = pl.BlockSpec(memory_space=pltpu.VMEM)
HBM = pl.BlockSpec(memory_space=pltpu.HBM)


def round_up(count, unit):
    return -(-count // unit) * unit


class Wire:
    def __init__(self, messages, capacity, width):
        self.messages = messages
        self.capacity = capacity
        self.pad = round_up(capacity, TILE_ROWS)
        self.lanes = LANES if width % LANES == 0 else width
        self.columns = width // self.lanes
        self.stride = round_up(self.columns * capacity, TILE_ROWS)
        self.rows = messages * self.stride

    def window(self, message, column):
        start = message * self.stride + column * self.capacity
        return slice(start, start + self.pad)

    def slot(self, message):
        return slice(message * self.pad, (message + 1) * self.pad)

    def block(self, column):
        return slice(column * self.lanes, (column + 1) * self.lanes)

    def scratch(self):
        return pltpu.VMEM((self.rows + self.pad, self.lanes), jnp.float32)

    def pack(self, scratch, out_refs, get):
        blank = jnp.zeros((TILE_ROWS, self.lanes), jnp.float32)
        for message in range(self.messages):
            end = (message + 1) * self.stride
            scratch[end - TILE_ROWS : end, :] = blank
            for column in range(self.columns):
                scratch[self.window(message, column), :] = get(message, column)
        part = self.rows // len(out_refs)
        for n, out_ref in enumerate(out_refs):
            out_ref[...] = scratch[n * part : (n + 1) * part, :].astype(jnp.bfloat16)

    def unpack(self, wire_refs, scratch, put):
        part = self.rows // len(wire_refs)
        for n, wire_ref in enumerate(wire_refs):
            scratch[n * part : (n + 1) * part, :] = wire_ref[...].astype(jnp.float32)
        scratch[self.rows :, :] = jnp.zeros((self.pad, self.lanes), jnp.float32)
        for message in range(self.messages):
            for column in range(self.columns):
                put(message, column, scratch[self.window(message, column), :].astype(jnp.bfloat16))


def dot(a, b):
    return jnp.dot(a, b, preferred_element_type=jnp.float32)


def pairwise(blocks):
    return blocks & (blocks - 1) == 0 and blocks <= MOST_EXCHANGES


def issue_order(blocks):
    half = blocks // 2
    bits = max(1, half.bit_length() - 1)
    far = sorted(range(half), key=lambda n: format(n, f"0{bits}b")[::-1])
    return [0, *(half + n for n in far), *range(half - 1, 0, -1)]


def gather_kernel(tok_hbm, gain_hbm, route_hbm, *rest, wire, order):
    *out_refs, tok_ref, gain_ref, route_ref, scratch, sems = rest
    tok_count, width = tok_ref.shape
    half = width // CORES
    copies = [
        pltpu.make_async_copy(source, target, sems.at[i])
        for i, (source, target) in enumerate(
            ((route_hbm, route_ref), (tok_hbm, tok_ref), (gain_hbm, gain_ref))
        )
    ]
    for copy in copies:
        copy.start()
    copies[0].wait()
    slots = wire.messages * wire.pad
    row = lax.broadcasted_iota(jnp.int32, (slots, tok_count), 0)
    message = row // wire.pad
    place = (row - message * wire.pad).astype(jnp.float32)
    expert = message
    if pairwise(wire.messages):
        expert = lax.bitwise_xor(message, lax.axis_index("ep"))
    chosen = functools.reduce(
        jnp.logical_or, [route_ref[k][None, :] == expert for k in range(route_ref.shape[0])]
    )
    earlier = lax.broadcasted_iota(jnp.int32, (tok_count, tok_count), 0) < lax.broadcasted_iota(
        jnp.int32, (tok_count, tok_count), 1
    )
    rank = dot(chosen.astype(jnp.bfloat16), earlier.astype(jnp.bfloat16))
    select = (chosen & (rank == place)).astype(jnp.bfloat16)
    copies[1].wait()
    values = tok_ref[...].astype(jnp.float32)
    scale = lax.rsqrt(jnp.mean(values * values, axis=-1, keepdims=True) + NORM_EPS)
    copies[2].wait()
    lanes = pl.ds(pl.multiple_of(lax.axis_index("core") * half, half), half)
    own = tok_ref[:, lanes].astype(jnp.float32)
    normal = (own * scale * gain_ref[:, lanes]).astype(jnp.bfloat16)
    rows = dot(select, normal)
    wire.pack(
        scratch,
        out_refs,
        lambda message, column: rows[wire.slot(order[message]), wire.block(column)],
    )


def arrange_kernel(*refs, wire, order):
    *wire_refs, x_ref, scratch = refs

    def put(message, column, rows):
        x_ref[wire.slot(order[message]), wire.block(column)] = rows

    wire.unpack(wire_refs, scratch, put)


def first_kernel(x_ref, gate_ref, up_ref, _, gate_out, up_out):
    half = x_ref.shape[1]
    rows = pl.ds(pl.multiple_of(lax.axis_index("core") * half, half), half)
    gate_out[...] = dot(x_ref[...], gate_ref[0, rows, :])
    up_out[...] = dot(x_ref[...], up_ref[0, rows, :])


def column_block(down_ref, group, core, width):
    if width % LANES == 0:
        start = (group * CORES + core) * width
        return down_ref[0, :, pl.ds(pl.multiple_of(start, width), width)]
    first, second = [
        down_ref[0, :, (group * CORES + i) * width : (group * CORES + i + 1) * width]
        for i in range(CORES)
    ]
    return jnp.where(core == 0, first, second)


def second_kernel(
    x_ref, gate_in, up_in, gate_ref, up_ref, down_ref, hidden_ref, away_ref
):
    half = x_ref.shape[1]
    other = (CORES - 1) - lax.axis_index("core")
    rows = pl.ds(pl.multiple_of(other * half, half), half)
    gate_pre = gate_in[...] + dot(x_ref[...], gate_ref[0, rows, :])
    up_pre = up_in[...] + dot(x_ref[...], up_ref[0, rows, :])
    gated = jnp.minimum(gate_pre, CLAMP_LIMIT)
    upper = jnp.clip(up_pre, -CLAMP_LIMIT, CLAMP_LIMIT)
    hidden = ((upper + 1.0) * gated * jax.nn.sigmoid(SIGMOID_SCALE * gated)).astype(jnp.bfloat16)
    hidden_ref[...] = hidden
    groups, _, width = away_ref.shape
    for group in range(groups):
        block = column_block(down_ref, group, other, width)
        away_ref[group] = dot(hidden, block).astype(jnp.bfloat16)


def turned(eye, table):
    return lax.dot_general(
        eye, table, (((1,), (1,)), ((), ())), preferred_element_type=jnp.float32
    )


def third_kernel(
    hidden_ref, down_ref, route_ref, weight_ref, own_ref, mix_ref, *, wire, experts
):
    groups, _, width = own_ref.shape
    for group in range(groups):
        block = column_block(down_ref, group, lax.axis_index("core"), width)
        own_ref[group] = dot(hidden_ref[...], block)

    bf16, f32 = jnp.bfloat16, jnp.float32
    top_count, tok_count = route_ref.shape
    square = (tok_count, tok_count)
    down_at = lax.broadcasted_iota(jnp.int32, square, 0)
    across = lax.broadcasted_iota(jnp.int32, square, 1)
    eye = (down_at == across).astype(bf16)
    routes = turned(eye, route_ref[...].astype(bf16)).astype(jnp.int32)
    weights = weight_ref[...]
    high = weights.astype(bf16)
    low = (weights - high.astype(f32)).astype(bf16)
    weights = turned(eye, high) + turned(eye, low)
    lane = lax.broadcasted_iota(jnp.int32, (1, wire.rows), 1)
    message = lane // wire.stride
    offset = (lane - message * wire.stride).astype(f32)
    expert = lax.rem(message, wire.messages // groups)
    weight = jnp.zeros((tok_count, wire.rows), f32)
    chosen = jnp.zeros((tok_count, wire.rows), f32)
    for k in range(top_count):
        at = routes[:, k : k + 1] == expert
        weight = jnp.where(at, weights[:, k : k + 1], weight)
        chosen = jnp.where(at, 1.0, chosen)
    rank = dot((across < down_at).astype(bf16), chosen.astype(bf16))
    away = offset - rank
    mix = jnp.concatenate(
        [
            jnp.where(away == float(column * wire.capacity), weight, 0.0)
            for column in range(wire.columns)
        ],
        axis=0,
    )
    high = mix.astype(bf16)
    mix_ref[0] = high
    mix_ref[1] = (mix - high.astype(f32)).astype(bf16)


def add_kernel(own_ref, away_ref, out_ref, scratch, *, wire):
    groups = own_ref.shape[0]
    blocks = wire.messages // groups

    def get(message, column):
        group, slot = divmod(message, blocks)
        if pairwise(blocks):
            slot = lax.bitwise_xor(slot, lax.axis_index("ep"))
        rows = pl.ds(pl.multiple_of(slot * wire.pad, wire.pad), wire.pad)
        lanes = wire.block(column)
        return own_ref[group, rows, lanes] + away_ref[group, rows, lanes].astype(jnp.float32)

    wire.pack(scratch, [out_ref], get)


def combine_kernel(back_ref, mix_ref, out_ref, *, wire):
    tok_count = out_ref.shape[0]
    total = dot(mix_ref[0], back_ref[...]) + dot(mix_ref[1], back_ref[...])
    for column in range(wire.columns):
        rows = total[column * tok_count : (column + 1) * tok_count]
        out_ref[:, wire.block(column)] = rows.astype(jnp.bfloat16)


def in_hbm(array):
    return pltpu.with_memory_space_constraint(array, pltpu.HBM)


def call(kernel, out_shape, args, flops, moved, scratch=(), spaces=None, limit=16 * MIB):
    specs = spaces or [VMEM] * len(args)
    return pl.pallas_call(
        kernel,
        out_shape=out_shape,
        in_specs=specs,
        out_specs=jax.tree.map(lambda _: VMEM, out_shape),
        scratch_shapes=scratch,
        compiler_params=pltpu.CompilerParams(vmem_limit_bytes=limit),
        cost_estimate=pl.CostEstimate(flops=flops, bytes_accessed=moved, transcendentals=0),
    )(*args)


def local(tokens, norm_gain, routing, route_weight, w_gate, w_up, w_down):
    tok_count, width = tokens.shape
    top_count = routing.shape[1]
    blocks = lax.axis_size("ep")
    groups = lax.axis_size("y")
    experts = blocks * w_gate.shape[0]
    hidden_width = w_gate.shape[2]
    capacity = max(2, tok_count * top_count // experts + 1)
    half = width // CORES
    share = width // (groups * CORES)
    there = Wire(blocks, capacity, half)
    home = Wire(blocks * groups, capacity, share)
    rows = blocks * there.pad
    swap = [(i, CORES - 1 - i) for i in range(CORES)]
    routes = routing.T
    weights = route_weight.T
    bf16, f32 = jnp.bfloat16, jnp.float32
    shape = jax.ShapeDtypeStruct

    direct = pairwise(blocks)
    parts = blocks if direct else 1
    order = issue_order(blocks) if direct else range(blocks)
    sending = call(
        functools.partial(gather_kernel, wire=there, order=order),
        (shape((there.rows // parts, there.lanes), bf16),) * parts,
        [in_hbm(a) for a in (tokens, norm_gain.reshape(1, width), routes)],
        40 * 10**9,
        60 * 10**6,
        scratch=(
            pltpu.VMEM((tok_count, width), bf16),
            pltpu.VMEM((1, width), f32),
            pltpu.VMEM((top_count, tok_count), jnp.int32),
            there.scratch(),
            pltpu.SemaphoreType.DMA((3,)),
        ),
        spaces=[HBM, HBM, HBM],
    )
    if direct:
        came = [sending[0]]
        for piece, mask in zip(sending[1:], order[1:]):
            came.append(lax.ppermute(piece, "ep", [(i, i ^ mask) for i in range(blocks)]))
    else:
        came = [
            lax.all_to_all(
                sending[0].reshape(blocks, there.stride, there.lanes),
                "ep",
                split_axis=0,
                concat_axis=0,
                tiled=True,
            ).reshape(there.rows, there.lanes)
        ]
    own = call(
        functools.partial(arrange_kernel, wire=there, order=order),
        shape((rows, half), bf16),
        came,
        rows * half,
        4 * rows * half,
        scratch=(there.scratch(),),
    )
    peer = lax.ppermute(own, "core", swap)
    pre = shape((rows, hidden_width), f32)
    step = 2 * rows * half * hidden_width
    gate_part, up_part = call(
        first_kernel,
        (pre, pre),
        (own, w_gate, w_up, w_down),
        2 * step,
        4 * half * hidden_width,
    )
    hidden, away = call(
        second_kernel,
        (shape((rows, hidden_width), bf16), shape((groups, rows, share), bf16)),
        (peer, gate_part, up_part, w_gate, w_up, w_down),
        3 * step,
        6 * half * hidden_width,
    )
    arrived = lax.ppermute(away, "core", swap)
    kept, mix = call(
        functools.partial(third_kernel, wire=home, experts=experts),
        (
            shape((groups, rows, share), f32),
            shape((2, home.columns * tok_count, home.rows), bf16),
        ),
        (hidden, w_down, routes, weights),
        step,
        2 * half * hidden_width,
    )
    summed = call(
        functools.partial(add_kernel, wire=home),
        shape((home.rows, home.lanes), bf16),
        (kept, arrived),
        rows * half,
        8 * rows * half,
        scratch=(home.scratch(),),
    )
    back = lax.all_to_all(
        summed.reshape(blocks * groups, home.stride, home.lanes),
        ("y", "ep"),
        split_axis=0,
        concat_axis=0,
        tiled=True,
    ).reshape(home.rows, home.lanes)
    return call(
        functools.partial(combine_kernel, wire=home),
        shape((tok_count, share), bf16),
        (back, mix),
        4 * rows * tok_count * half,
        4 * rows * half,
    )


def solution(mesh):
    blocks, shares = mesh.devices.shape
    split = Mesh(mesh.devices.reshape(blocks, shares // CORES, CORES), ("ep", "y", "core"))
    tp = ("y", "core")
    placed = (
        P("ep", None),
        P(),
        P("ep", None),
        P("ep", None),
        P("ep", None, tp),
        P("ep", None, tp),
        P("ep", tp, None),
    )
    return jax.shard_map(
        local, mesh=split, in_specs=placed, out_specs=P("ep", tp), check_vma=False
    )
```

```python
import functools

import jax
import jax.numpy as jnp
from jax import lax
from jax.experimental import pallas as pl
from jax.experimental.pallas import tpu as pltpu
from jax.sharding import Mesh, PartitionSpec as P

NORM_EPS = 1e-06
CLAMP_LIMIT = 7.0
SIGMOID_SCALE = 1.702
CORES = 2
TILE_ROWS = 16
LANES = 128
MIB = 1 << 20

VMEM = pl.BlockSpec(memory_space=pltpu.VMEM)
HBM = pl.BlockSpec(memory_space=pltpu.HBM)


def round_up(count, unit):
    return -(-count // unit) * unit


class Wire:
    def __init__(self, messages, capacity, width):
        self.messages = messages
        self.capacity = capacity
        self.pad = round_up(capacity, TILE_ROWS)
        self.lanes = LANES if width % LANES == 0 else width
        self.columns = width // self.lanes
        self.stride = round_up(self.columns * capacity, TILE_ROWS)
        self.rows = messages * self.stride

    def window(self, message, column):
        start = message * self.stride + column * self.capacity
        return slice(start, start + self.pad)

    def slot(self, message):
        return slice(message * self.pad, (message + 1) * self.pad)

    def block(self, column):
        return slice(column * self.lanes, (column + 1) * self.lanes)

    def scratch(self):
        return pltpu.VMEM((self.rows + self.pad, self.lanes), jnp.float32)

    def pack(self, scratch, out_refs, get):
        blank = jnp.zeros((TILE_ROWS, self.lanes), jnp.float32)
        for message in range(self.messages):
            end = (message + 1) * self.stride
            scratch[end - TILE_ROWS : end, :] = blank
            for column in range(self.columns):
                scratch[self.window(message, column), :] = get(message, column)
        part = self.rows // len(out_refs)
        for n, out_ref in enumerate(out_refs):
            out_ref[...] = scratch[n * part : (n + 1) * part, :].astype(jnp.bfloat16)

    def unpack(self, wire_refs, scratch, put):
        part = self.rows // len(wire_refs)
        for n, wire_ref in enumerate(wire_refs):
            scratch[n * part : (n + 1) * part, :] = wire_ref[...].astype(jnp.float32)
        scratch[self.rows :, :] = jnp.zeros((self.pad, self.lanes), jnp.float32)
        for message in range(self.messages):
            for column in range(self.columns):
                put(message, column, scratch[self.window(message, column), :].astype(jnp.bfloat16))


def dot(a, b):
    return jnp.dot(a, b, preferred_element_type=jnp.float32)


def joined(place, step, count):
    if count & (count - 1) == 0:
        return place ^ step
    moved = place + step
    return moved - count * (moved >= count)


def step_from(place, source, count):
    if count & (count - 1) == 0:
        return place ^ source
    moved = place - source
    return moved + count * (moved < 0)


def rounds_of(count):
    half = count // 2
    bits = max(1, half.bit_length() - 1)
    far = sorted(range(half), key=lambda n: format(n, f"0{bits}b")[::-1])
    rest = range(half - 1, 0, -1)
    if count & (count - 1):
        far, half, rest = range(1, count), 0, ()
    steps = [*(half + n for n in far), *rest]
    steps += [0] * (-len(steps) % CORES)
    return [steps[at : at + CORES][::-1] for at in range(0, len(steps), CORES)]


def by_core(steps):
    core = lax.axis_index("core")
    return functools.reduce(
        lambda chosen, at: jnp.where(core == at, steps[at], chosen), range(1, CORES), steps[0]
    )


def gather_kernel(tok_hbm, gain_hbm, route_hbm, *rest, wire, rounds, count):
    own_ref, *out_refs, tok_ref, gain_ref, route_ref, scratch, sems = rest
    tok_count = tok_ref.shape[0]
    copies = [
        pltpu.make_async_copy(source, target, sems.at[i])
        for i, (source, target) in enumerate(
            ((route_hbm, route_ref), (tok_hbm, tok_ref), (gain_hbm, gain_ref))
        )
    ]
    for copy in copies:
        copy.start()
    copies[0].wait()
    me = lax.axis_index("ep")
    slots = (len(rounds) + 1) * wire.pad
    row = lax.broadcasted_iota(jnp.int32, (slots, tok_count), 0)
    message = row // wire.pad
    place = (row - message * wire.pad).astype(jnp.float32)
    expert = jnp.full((slots, tok_count), me, jnp.int32)
    for n, steps in enumerate(rounds):
        step = by_core(steps)
        target = jnp.where(step == 0, -1, joined(me, step, count))
        expert = jnp.where(message == n + 1, target, expert)
    chosen = functools.reduce(
        jnp.logical_or, [route_ref[k][None, :] == expert for k in range(route_ref.shape[0])]
    )
    earlier = lax.broadcasted_iota(jnp.int32, (tok_count, tok_count), 0) < lax.broadcasted_iota(
        jnp.int32, (tok_count, tok_count), 1
    )
    rank = dot(chosen.astype(jnp.bfloat16), earlier.astype(jnp.bfloat16))
    select = (chosen & (rank == place)).astype(jnp.bfloat16)
    copies[1].wait()
    values = tok_ref[...].astype(jnp.float32)
    scale = lax.rsqrt(jnp.mean(values * values, axis=-1, keepdims=True) + NORM_EPS)
    copies[2].wait()
    normal = (values * scale * gain_ref[...]).astype(jnp.bfloat16)
    rows = dot(select, normal)
    own_ref[...] = rows[: wire.pad].astype(jnp.bfloat16)
    wire.pack(
        scratch,
        out_refs,
        lambda message, column: rows[wire.slot(message + 1), wire.block(column)],
    )


def arrange_kernel(*refs, wire):
    *wire_refs, x_ref, scratch = refs

    def put(message, column, rows):
        x_ref[wire.slot(message), wire.block(column)] = rows

    wire.unpack(wire_refs, scratch, put)


def unit(gate_pre, up_pre):
    gated = jnp.minimum(gate_pre, CLAMP_LIMIT)
    upper = jnp.clip(up_pre, -CLAMP_LIMIT, CLAMP_LIMIT)
    return ((upper + 1.0) * gated * jax.nn.sigmoid(SIGMOID_SCALE * gated)).astype(jnp.bfloat16)


def column_block(down_ref, group, core, width):
    if width % LANES == 0:
        start = (group * CORES + core) * width
        return down_ref[0, :, pl.ds(pl.multiple_of(start, width), width)]
    first, second = [
        down_ref[0, :, (group * CORES + i) * width : (group * CORES + i + 1) * width]
        for i in range(CORES)
    ]
    return jnp.where(core == 0, first, second)


def expert_kernel(
    own_ref, near_ref, peer_ref, gate_ref, up_ref, down_ref, hidden_ref, away_ref, x_ref
):
    start = 0
    for ref in (own_ref, near_ref, peer_ref):
        x_ref[start : start + ref.shape[0]] = ref[...]
        start += ref.shape[0]
    hidden_ref[...] = unit(dot(x_ref[...], gate_ref[0]), dot(x_ref[...], up_ref[0]))
    other = (CORES - 1) - lax.axis_index("core")
    groups, _, width = away_ref.shape
    for group in range(groups):
        block = column_block(down_ref, group, other, width)
        away_ref[group] = dot(hidden_ref[...], block).astype(jnp.bfloat16)


def turned(eye, table):
    return lax.dot_general(
        eye, table, (((1,), (1,)), ((), ())), preferred_element_type=jnp.float32
    )


def third_kernel(
    hidden_ref, down_ref, route_ref, weight_ref, own_ref, mix_ref, *, wire, experts
):
    groups, _, width = own_ref.shape
    for group in range(groups):
        block = column_block(down_ref, group, lax.axis_index("core"), width)
        own_ref[group] = dot(hidden_ref[...], block)

    bf16, f32 = jnp.bfloat16, jnp.float32
    top_count, tok_count = route_ref.shape
    square = (tok_count, tok_count)
    down_at = lax.broadcasted_iota(jnp.int32, square, 0)
    across = lax.broadcasted_iota(jnp.int32, square, 1)
    eye = (down_at == across).astype(bf16)
    routes = turned(eye, route_ref[...].astype(bf16)).astype(jnp.int32)
    weights = weight_ref[...]
    high = weights.astype(bf16)
    low = (weights - high.astype(f32)).astype(bf16)
    weights = turned(eye, high) + turned(eye, low)
    lane = lax.broadcasted_iota(jnp.int32, (1, wire.rows), 1)
    message = lane // wire.stride
    offset = (lane - message * wire.stride).astype(f32)
    expert = lax.rem(message, wire.messages // groups)
    weight = jnp.zeros((tok_count, wire.rows), f32)
    chosen = jnp.zeros((tok_count, wire.rows), f32)
    for k in range(top_count):
        at = routes[:, k : k + 1] == expert
        weight = jnp.where(at, weights[:, k : k + 1], weight)
        chosen = jnp.where(at, 1.0, chosen)
    rank = dot((across < down_at).astype(bf16), chosen.astype(bf16))
    away = offset - rank
    mix = jnp.concatenate(
        [
            jnp.where(away == float(column * wire.capacity), weight, 0.0)
            for column in range(wire.columns)
        ],
        axis=0,
    )
    high = mix.astype(bf16)
    mix_ref[0] = high
    mix_ref[1] = (mix - high.astype(f32)).astype(bf16)


def slot_of(block, core, rounds, count):
    step = step_from(lax.axis_index("ep"), block, count)
    slot = jnp.int32(0)
    for n, steps in enumerate(rounds):
        for at in range(CORES):
            if steps[at]:
                here = jnp.where(core == at, 1 + n, 1 + len(rounds) + n)
                slot = jnp.where(step == steps[at], here, slot)
    return slot


def add_kernel(own_ref, away_ref, out_ref, scratch, *, wire, rounds):
    groups = own_ref.shape[0]
    blocks = wire.messages // groups
    core = lax.axis_index("core")

    def starts(core):
        return [
            pl.multiple_of(slot_of(block, core, rounds, blocks) * wire.pad, wire.pad)
            for block in range(blocks)
        ]

    here, there = starts(core), starts((CORES - 1) - core)

    def get(message, column):
        group, block = divmod(message, blocks)
        rows = pl.ds(here[block], wire.pad)
        theirs = pl.ds(there[block], wire.pad)
        lanes = wire.block(column)
        return own_ref[group, rows, lanes] + away_ref[group, theirs, lanes].astype(
            jnp.float32
        )

    wire.pack(scratch, [out_ref], get)


def combine_kernel(back_ref, mix_ref, out_ref, *, wire):
    tok_count = out_ref.shape[0]
    total = dot(mix_ref[0], back_ref[...]) + dot(mix_ref[1], back_ref[...])
    for column in range(wire.columns):
        rows = total[column * tok_count : (column + 1) * tok_count]
        out_ref[:, wire.block(column)] = rows.astype(jnp.bfloat16)


def in_hbm(array):
    return pltpu.with_memory_space_constraint(array, pltpu.HBM)


def call(kernel, out_shape, args, flops, moved, scratch=(), spaces=None, limit=16 * MIB):
    specs = spaces or [VMEM] * len(args)
    return pl.pallas_call(
        kernel,
        out_shape=out_shape,
        in_specs=specs,
        out_specs=jax.tree.map(lambda _: VMEM, out_shape),
        scratch_shapes=scratch,
        compiler_params=pltpu.CompilerParams(vmem_limit_bytes=limit),
        cost_estimate=pl.CostEstimate(flops=flops, bytes_accessed=moved, transcendentals=0),
    )(*args)


def local(tokens, norm_gain, routing, route_weight, w_gate, w_up, w_down):
    tok_count, width = tokens.shape
    top_count = routing.shape[1]
    blocks = lax.axis_size("ep")
    groups = lax.axis_size("y")
    experts = blocks * w_gate.shape[0]
    hidden_width = w_gate.shape[2]
    capacity = max(2, tok_count * top_count // experts + 1)
    half = width // CORES
    share = width // (groups * CORES)
    rounds = rounds_of(blocks)
    there = Wire(len(rounds), capacity, width)
    home = Wire(blocks * groups, capacity, share)
    rows = (1 + CORES * len(rounds)) * there.pad
    swap = [(i, CORES - 1 - i) for i in range(CORES)]
    routes = routing.T
    weights = route_weight.T
    bf16, f32 = jnp.bfloat16, jnp.float32
    shape = jax.ShapeDtypeStruct

    sending = call(
        functools.partial(gather_kernel, wire=there, rounds=rounds, count=blocks),
        (shape((there.pad, width), bf16),)
        + (shape((there.stride, there.lanes), bf16),) * len(rounds),
        [in_hbm(a) for a in (tokens, norm_gain.reshape(1, width), routes)],
        40 * 10**9,
        60 * 10**6,
        scratch=(
            pltpu.VMEM((tok_count, width), bf16),
            pltpu.VMEM((1, width), f32),
            pltpu.VMEM((top_count, tok_count), jnp.int32),
            there.scratch(),
            pltpu.SemaphoreType.DMA((3,)),
        ),
        spaces=[HBM, HBM, HBM],
    )
    came = []
    for steps, piece in zip(rounds, sending[1:]):
        pairs = [
            (place * CORES + at, joined(place, steps[at], blocks) * CORES + at)
            for place in range(blocks)
            for at in range(CORES)
        ]
        came.append(lax.ppermute(piece, ("ep", "core"), pairs))
    near = call(
        functools.partial(arrange_kernel, wire=there),
        shape((len(rounds) * there.pad, width), bf16),
        came,
        rows * half,
        4 * rows * half,
        scratch=(there.scratch(),),
    )
    peer = lax.ppermute(near, "core", swap)
    step = 2 * rows * half * hidden_width
    hidden, away = call(
        expert_kernel,
        (shape((rows, hidden_width), bf16), shape((groups, rows, share), bf16)),
        (sending[0], near, peer, w_gate, w_up, w_down),
        5 * step,
        6 * width * hidden_width,
        scratch=(pltpu.VMEM((rows, width), bf16),),
    )
    arrived = lax.ppermute(away, "core", swap)
    kept, mix = call(
        functools.partial(third_kernel, wire=home, experts=experts),
        (
            shape((groups, rows, share), f32),
            shape((2, home.columns * tok_count, home.rows), bf16),
        ),
        (hidden, w_down, routes, weights),
        step,
        2 * half * hidden_width,
    )
    summed = call(
        functools.partial(add_kernel, wire=home, rounds=rounds),
        shape((home.rows, home.lanes), bf16),
        (kept, arrived),
        rows * half,
        8 * rows * half,
        scratch=(home.scratch(),),
    )
    back = lax.all_to_all(
        summed.reshape(blocks * groups, home.stride, home.lanes),
        ("y", "ep"),
        split_axis=0,
        concat_axis=0,
        tiled=True,
    ).reshape(home.rows, home.lanes)
    return call(
        functools.partial(combine_kernel, wire=home),
        shape((tok_count, share), bf16),
        (back, mix),
        4 * rows * tok_count * half,
        4 * rows * half,
    )


def solution(mesh):
    blocks, shares = mesh.devices.shape
    split = Mesh(mesh.devices.reshape(blocks, shares // CORES, CORES), ("ep", "y", "core"))
    tp = ("y", "core")
    placed = (
        P("ep", None),
        P(),
        P("ep", None),
        P("ep", None),
        P("ep", None, tp),
        P("ep", None, tp),
        P("ep", tp, None),
    )
    return jax.shard_map(
        local, mesh=split, in_specs=placed, out_specs=P("ep", tp), check_vma=False
    )
```

```python
import functools

import jax
import jax.numpy as jnp
from jax import lax
from jax.experimental import pallas as pl
from jax.experimental.pallas import tpu as pltpu
from jax.sharding import Mesh, PartitionSpec as P

NORM_EPS = 1e-06
CLAMP_LIMIT = 7.0
SIGMOID_SCALE = 1.702
CORES = 2
TILE_ROWS = 16
LANES = 128
MIB = 1 << 20

VMEM = pl.BlockSpec(memory_space=pltpu.VMEM)
HBM = pl.BlockSpec(memory_space=pltpu.HBM)


def round_up(count, unit):
    return -(-count // unit) * unit


class Wire:
    def __init__(self, messages, capacity, width):
        self.messages = messages
        self.capacity = capacity
        self.pad = round_up(capacity, TILE_ROWS)
        self.lanes = LANES if width % LANES == 0 else width
        self.columns = width // self.lanes
        self.stride = round_up(self.columns * capacity, TILE_ROWS)
        self.rows = messages * self.stride

    def window(self, message, column):
        start = message * self.stride + column * self.capacity
        return slice(start, start + self.pad)

    def slot(self, message):
        return slice(message * self.pad, (message + 1) * self.pad)

    def block(self, column):
        return slice(column * self.lanes, (column + 1) * self.lanes)

    def scratch(self):
        return pltpu.VMEM((self.rows + self.pad, self.lanes), jnp.float32)

    def pack(self, scratch, out_refs, get):
        blank = jnp.zeros((TILE_ROWS, self.lanes), jnp.float32)
        for message in range(self.messages):
            end = (message + 1) * self.stride
            scratch[end - TILE_ROWS : end, :] = blank
            for column in range(self.columns):
                scratch[self.window(message, column), :] = get(message, column)
        part = self.rows // len(out_refs)
        for n, out_ref in enumerate(out_refs):
            out_ref[...] = scratch[n * part : (n + 1) * part, :].astype(jnp.bfloat16)

    def unpack(self, wire_refs, scratch, put):
        part = self.rows // len(wire_refs)
        for n, wire_ref in enumerate(wire_refs):
            scratch[n * part : (n + 1) * part, :] = wire_ref[...].astype(jnp.float32)
        scratch[self.rows :, :] = jnp.zeros((self.pad, self.lanes), jnp.float32)
        for message in range(self.messages):
            for column in range(self.columns):
                put(message, column, scratch[self.window(message, column), :].astype(jnp.bfloat16))


def dot(a, b):
    return jnp.dot(a, b, preferred_element_type=jnp.float32)


def joined(place, step, count):
    if count & (count - 1) == 0:
        return place ^ step
    moved = place + step
    return moved - count * (moved >= count)


def step_from(place, source, count):
    if count & (count - 1) == 0:
        return place ^ source
    moved = place - source
    return moved + count * (moved < 0)


def rounds_of(count):
    half = count // 2
    if count & (count - 1) or half % 4:
        steps = [*range(1, count)] + [0] * ((1 - count) % CORES)
    else:
        fours = range(0, half, 4)
        steps = [half + base + n for base in fours for n in (1, 3, 2, 0)]
        steps += [base + n for base in fours for n in (1, 3, 0, 2)]
    return [steps[at : at + CORES] for at in range(0, len(steps), CORES)]


def by_core(steps):
    core = lax.axis_index("core")
    return functools.reduce(
        lambda chosen, at: jnp.where(core == at, steps[at], chosen), range(1, CORES), steps[0]
    )


def gather_kernel(tok_hbm, gain_hbm, route_hbm, *rest, wire, rounds, count):
    own_ref, *out_refs, tok_ref, gain_ref, route_ref, scratch, sems = rest
    tok_count = tok_ref.shape[0]
    copies = [
        pltpu.make_async_copy(source, target, sems.at[i])
        for i, (source, target) in enumerate(
            ((route_hbm, route_ref), (tok_hbm, tok_ref), (gain_hbm, gain_ref))
        )
    ]
    for copy in copies:
        copy.start()
    copies[0].wait()
    me = lax.axis_index("ep")
    slots = (len(rounds) + 1) * wire.pad
    row = lax.broadcasted_iota(jnp.int32, (slots, tok_count), 0)
    message = row // wire.pad
    place = (row - message * wire.pad).astype(jnp.float32)
    expert = jnp.full((slots, tok_count), me, jnp.int32)
    for n, steps in enumerate(rounds):
        step = by_core(steps)
        target = jnp.where(step == 0, -1, joined(me, step, count))
        expert = jnp.where(message == n + 1, target, expert)
    chosen = functools.reduce(
        jnp.logical_or, [route_ref[k][None, :] == expert for k in range(route_ref.shape[0])]
    )
    earlier = lax.broadcasted_iota(jnp.int32, (tok_count, tok_count), 0) < lax.broadcasted_iota(
        jnp.int32, (tok_count, tok_count), 1
    )
    rank = dot(chosen.astype(jnp.bfloat16), earlier.astype(jnp.bfloat16))
    select = (chosen & (rank == place)).astype(jnp.bfloat16)
    copies[1].wait()
    values = tok_ref[...].astype(jnp.float32)
    scale = lax.rsqrt(jnp.mean(values * values, axis=-1, keepdims=True) + NORM_EPS)
    copies[2].wait()
    normal = (values * scale * gain_ref[...]).astype(jnp.bfloat16)
    rows = dot(select, normal)
    own_ref[...] = rows[: wire.pad].astype(jnp.bfloat16)
    wire.pack(
        scratch,
        out_refs,
        lambda message, column: rows[wire.slot(message + 1), wire.block(column)],
    )


def arrange_kernel(*refs, wire):
    *wire_refs, x_ref, scratch = refs

    def put(message, column, rows):
        x_ref[wire.slot(message), wire.block(column)] = rows

    wire.unpack(wire_refs, scratch, put)


def unit(gate_pre, up_pre):
    gated = jnp.minimum(gate_pre, CLAMP_LIMIT)
    upper = jnp.clip(up_pre, -CLAMP_LIMIT, CLAMP_LIMIT)
    return ((upper + 1.0) * gated * jax.nn.sigmoid(SIGMOID_SCALE * gated)).astype(jnp.bfloat16)


def column_block(down_ref, group, core, width):
    if width % LANES == 0:
        start = (group * CORES + core) * width
        return down_ref[0, :, pl.ds(pl.multiple_of(start, width), width)]
    first, second = [
        down_ref[0, :, (group * CORES + i) * width : (group * CORES + i + 1) * width]
        for i in range(CORES)
    ]
    return jnp.where(core == 0, first, second)


def expert_kernel(
    own_ref, near_ref, peer_ref, gate_ref, up_ref, down_ref, hidden_ref, away_ref, x_ref
):
    start = 0
    for ref in (own_ref, near_ref, peer_ref):
        x_ref[start : start + ref.shape[0]] = ref[...]
        start += ref.shape[0]
    hidden_ref[...] = unit(dot(x_ref[...], gate_ref[0]), dot(x_ref[...], up_ref[0]))
    other = (CORES - 1) - lax.axis_index("core")
    groups, _, width = away_ref.shape
    for group in range(groups):
        block = column_block(down_ref, group, other, width)
        away_ref[group] = dot(hidden_ref[...], block).astype(jnp.bfloat16)


def turned(eye, table):
    return lax.dot_general(
        eye, table, (((1,), (1,)), ((), ())), preferred_element_type=jnp.float32
    )


def third_kernel(
    hidden_ref, down_ref, route_ref, weight_ref, own_ref, mix_ref, *, wire, experts
):
    groups, _, width = own_ref.shape
    for group in range(groups):
        block = column_block(down_ref, group, lax.axis_index("core"), width)
        own_ref[group] = dot(hidden_ref[...], block)

    bf16, f32 = jnp.bfloat16, jnp.float32
    top_count, tok_count = route_ref.shape
    square = (tok_count, tok_count)
    down_at = lax.broadcasted_iota(jnp.int32, square, 0)
    across = lax.broadcasted_iota(jnp.int32, square, 1)
    eye = (down_at == across).astype(bf16)
    routes = turned(eye, route_ref[...].astype(bf16)).astype(jnp.int32)
    weights = weight_ref[...]
    high = weights.astype(bf16)
    low = (weights - high.astype(f32)).astype(bf16)
    weights = turned(eye, high) + turned(eye, low)
    lane = lax.broadcasted_iota(jnp.int32, (1, wire.rows), 1)
    message = lane // wire.stride
    offset = (lane - message * wire.stride).astype(f32)
    expert = lax.rem(message, wire.messages // groups)
    weight = jnp.zeros((tok_count, wire.rows), f32)
    chosen = jnp.zeros((tok_count, wire.rows), f32)
    for k in range(top_count):
        at = routes[:, k : k + 1] == expert
        weight = jnp.where(at, weights[:, k : k + 1], weight)
        chosen = jnp.where(at, 1.0, chosen)
    rank = dot((across < down_at).astype(bf16), chosen.astype(bf16))
    away = offset - rank
    mix = jnp.concatenate(
        [
            jnp.where(away == float(column * wire.capacity), weight, 0.0)
            for column in range(wire.columns)
        ],
        axis=0,
    )
    high = mix.astype(bf16)
    mix_ref[0] = high
    mix_ref[1] = (mix - high.astype(f32)).astype(bf16)


def slot_of(block, core, rounds, count):
    step = step_from(lax.axis_index("ep"), block, count)
    slot = jnp.int32(0)
    for n, steps in enumerate(rounds):
        for at in range(CORES):
            if steps[at]:
                here = jnp.where(core == at, 1 + n, 1 + len(rounds) + n)
                slot = jnp.where(step == steps[at], here, slot)
    return slot


def add_kernel(own_ref, away_ref, out_ref, scratch, *, wire, rounds):
    groups = own_ref.shape[0]
    blocks = wire.messages // groups
    core = lax.axis_index("core")

    def starts(core):
        return [
            pl.multiple_of(slot_of(block, core, rounds, blocks) * wire.pad, wire.pad)
            for block in range(blocks)
        ]

    here, there = starts(core), starts((CORES - 1) - core)

    def get(message, column):
        group, block = divmod(message, blocks)
        rows = pl.ds(here[block], wire.pad)
        theirs = pl.ds(there[block], wire.pad)
        lanes = wire.block(column)
        return own_ref[group, rows, lanes] + away_ref[group, theirs, lanes].astype(
            jnp.float32
        )

    wire.pack(scratch, [out_ref], get)


def combine_kernel(back_ref, mix_ref, out_ref, *, wire):
    tok_count = out_ref.shape[0]
    total = dot(mix_ref[0], back_ref[...]) + dot(mix_ref[1], back_ref[...])
    for column in range(wire.columns):
        rows = total[column * tok_count : (column + 1) * tok_count]
        out_ref[:, wire.block(column)] = rows.astype(jnp.bfloat16)


def in_hbm(array):
    return pltpu.with_memory_space_constraint(array, pltpu.HBM)


def call(kernel, out_shape, args, flops, moved, scratch=(), spaces=None, limit=16 * MIB):
    specs = spaces or [VMEM] * len(args)
    return pl.pallas_call(
        kernel,
        out_shape=out_shape,
        in_specs=specs,
        out_specs=jax.tree.map(lambda _: VMEM, out_shape),
        scratch_shapes=scratch,
        compiler_params=pltpu.CompilerParams(vmem_limit_bytes=limit),
        cost_estimate=pl.CostEstimate(flops=flops, bytes_accessed=moved, transcendentals=0),
    )(*args)


def local(tokens, norm_gain, routing, route_weight, w_gate, w_up, w_down):
    tok_count, width = tokens.shape
    top_count = routing.shape[1]
    blocks = lax.axis_size("ep")
    groups = lax.axis_size("y")
    experts = blocks * w_gate.shape[0]
    hidden_width = w_gate.shape[2]
    capacity = max(2, tok_count * top_count // experts + 1)
    half = width // CORES
    share = width // (groups * CORES)
    rounds = rounds_of(blocks)
    there = Wire(len(rounds), capacity, width)
    home = Wire(blocks * groups, capacity, share)
    rows = (1 + CORES * len(rounds)) * there.pad
    swap = [(i, CORES - 1 - i) for i in range(CORES)]
    routes = routing.T
    weights = route_weight.T
    bf16, f32 = jnp.bfloat16, jnp.float32
    shape = jax.ShapeDtypeStruct

    sending = call(
        functools.partial(gather_kernel, wire=there, rounds=rounds, count=blocks),
        (shape((there.pad, width), bf16),)
        + (shape((there.stride, there.lanes), bf16),) * len(rounds),
        [in_hbm(a) for a in (tokens, norm_gain.reshape(1, width), routes)],
        40 * 10**9,
        60 * 10**6,
        scratch=(
            pltpu.VMEM((tok_count, width), bf16),
            pltpu.VMEM((1, width), f32),
            pltpu.VMEM((top_count, tok_count), jnp.int32),
            there.scratch(),
            pltpu.SemaphoreType.DMA((3,)),
        ),
        spaces=[HBM, HBM, HBM],
    )
    came = []
    for steps, piece in zip(rounds, sending[1:]):
        pairs = [
            (place * CORES + at, joined(place, steps[at], blocks) * CORES + at)
            for place in range(blocks)
            for at in range(CORES)
        ]
        came.append(lax.ppermute(piece, ("ep", "core"), pairs))
    near = call(
        functools.partial(arrange_kernel, wire=there),
        shape((len(rounds) * there.pad, width), bf16),
        came,
        rows * half,
        4 * rows * half,
        scratch=(there.scratch(),),
    )
    peer = lax.ppermute(near, "core", swap)
    step = 2 * rows * half * hidden_width
    hidden, away = call(
        expert_kernel,
        (shape((rows, hidden_width), bf16), shape((groups, rows, share), bf16)),
        (sending[0], near, peer, w_gate, w_up, w_down),
        5 * step,
        6 * width * hidden_width,
        scratch=(pltpu.VMEM((rows, width), bf16),),
    )
    arrived = lax.ppermute(away, "core", swap)
    kept, mix = call(
        functools.partial(third_kernel, wire=home, experts=experts),
        (
            shape((groups, rows, share), f32),
            shape((2, home.columns * tok_count, home.rows), bf16),
        ),
        (hidden, w_down, routes, weights),
        step,
        2 * half * hidden_width,
    )
    summed = call(
        functools.partial(add_kernel, wire=home, rounds=rounds),
        shape((home.rows, home.lanes), bf16),
        (kept, arrived),
        rows * half,
        8 * rows * half,
        scratch=(home.scratch(),),
    )
    back = lax.all_to_all(
        summed.reshape(blocks * groups, home.stride, home.lanes),
        ("y", "ep"),
        split_axis=0,
        concat_axis=0,
        tiled=True,
    ).reshape(home.rows, home.lanes)
    return call(
        functools.partial(combine_kernel, wire=home),
        shape((tok_count, share), bf16),
        (back, mix),
        4 * rows * tok_count * half,
        4 * rows * half,
    )


def solution(mesh):
    blocks, shares = mesh.devices.shape
    split = Mesh(mesh.devices.reshape(blocks, shares // CORES, CORES), ("ep", "y", "core"))
    tp = ("y", "core")
    placed = (
        P("ep", None),
        P(),
        P("ep", None),
        P("ep", None),
        P("ep", None, tp),
        P("ep", None, tp),
        P("ep", tp, None),
    )
    return jax.shard_map(
        local, mesh=split, in_specs=placed, out_specs=P("ep", tp), check_vma=False
    )
```

```python
import functools

import jax
import jax.numpy as jnp
from jax import lax
from jax.experimental import pallas as pl
from jax.experimental.pallas import tpu as pltpu
from jax.sharding import Mesh, PartitionSpec as P

NORM_EPS = 1e-06
CLAMP_LIMIT = 7.0
SIGMOID_SCALE = 1.702
CORES = 2
BATCHES = 2
TILE_ROWS = 16
LANES = 128
MIB = 1 << 20

VMEM = pl.BlockSpec(memory_space=pltpu.VMEM)
HBM = pl.BlockSpec(memory_space=pltpu.HBM)


def round_up(count, unit):
    return -(-count // unit) * unit


class Wire:
    def __init__(self, messages, capacity, width):
        self.messages = messages
        self.capacity = capacity
        self.pad = round_up(capacity, TILE_ROWS)
        self.lanes = LANES if width % LANES == 0 else width
        self.columns = width // self.lanes
        self.stride = round_up(self.columns * capacity, TILE_ROWS)
        self.rows = messages * self.stride

    def window(self, message, column):
        start = message * self.stride + column * self.capacity
        return slice(start, start + self.pad)

    def slot(self, message):
        return slice(message * self.pad, (message + 1) * self.pad)

    def block(self, column):
        return slice(column * self.lanes, (column + 1) * self.lanes)

    def scratch(self):
        return pltpu.VMEM((self.rows + self.pad, self.lanes), jnp.float32)

    def pack(self, scratch, out_refs, get):
        blank = jnp.zeros((TILE_ROWS, self.lanes), jnp.float32)
        for message in range(self.messages):
            end = (message + 1) * self.stride
            scratch[end - TILE_ROWS : end, :] = blank
            for column in range(self.columns):
                scratch[self.window(message, column), :] = get(message, column)
        part = self.rows // len(out_refs)
        for n, out_ref in enumerate(out_refs):
            out_ref[...] = scratch[n * part : (n + 1) * part, :].astype(jnp.bfloat16)

    def unpack(self, wire_refs, scratch, put):
        part = self.rows // len(wire_refs)
        for n, wire_ref in enumerate(wire_refs):
            scratch[n * part : (n + 1) * part, :] = wire_ref[...].astype(jnp.float32)
        scratch[self.rows :, :] = jnp.zeros((self.pad, self.lanes), jnp.float32)
        for message in range(self.messages):
            for column in range(self.columns):
                put(message, column, scratch[self.window(message, column), :].astype(jnp.bfloat16))


def dot(a, b):
    return jnp.dot(a, b, preferred_element_type=jnp.float32)


def joined(place, step, count):
    if count & (count - 1) == 0:
        return place ^ step
    moved = place + step
    return moved - count * (moved >= count)


def step_from(place, source, count):
    if count & (count - 1) == 0:
        return place ^ source
    moved = place - source
    return moved + count * (moved < 0)


def rounds_of(count):
    half = count // 2
    if count & (count - 1) or half % 4:
        steps = [*range(1, count)] + [0] * ((1 - count) % CORES)
    else:
        fours = range(0, half, 4)
        steps = [half + base + n for base in fours for n in (1, 3, 2, 0)]
        steps += [base + n for base in fours for n in (1, 3, 0, 2)]
    return [steps[at : at + CORES] for at in range(0, len(steps), CORES)]


def by_core(steps):
    core = lax.axis_index("core")
    return functools.reduce(
        lambda chosen, at: jnp.where(core == at, steps[at], chosen), range(1, CORES), steps[0]
    )


def gather_kernel(tok_hbm, gain_hbm, route_hbm, *rest, wire, rounds, count):
    own_ref, *out_refs, tok_ref, gain_ref, route_ref, scratch, sems = rest
    tok_count = tok_ref.shape[0]
    copies = [
        pltpu.make_async_copy(source, target, sems.at[i])
        for i, (source, target) in enumerate(
            ((route_hbm, route_ref), (tok_hbm, tok_ref), (gain_hbm, gain_ref))
        )
    ]
    for copy in copies:
        copy.start()
    copies[0].wait()
    me = lax.axis_index("ep")
    slots = (len(rounds) + 1) * wire.pad
    row = lax.broadcasted_iota(jnp.int32, (slots, tok_count), 0)
    message = row // wire.pad
    place = (row - message * wire.pad).astype(jnp.float32)
    expert = jnp.full((slots, tok_count), me, jnp.int32)
    for n, steps in enumerate(rounds):
        step = by_core(steps)
        target = jnp.where(step == 0, -1, joined(me, step, count))
        expert = jnp.where(message == n + 1, target, expert)
    chosen = functools.reduce(
        jnp.logical_or, [route_ref[k][None, :] == expert for k in range(route_ref.shape[0])]
    )
    earlier = lax.broadcasted_iota(jnp.int32, (tok_count, tok_count), 0) < lax.broadcasted_iota(
        jnp.int32, (tok_count, tok_count), 1
    )
    rank = dot(chosen.astype(jnp.bfloat16), earlier.astype(jnp.bfloat16))
    select = (chosen & (rank == place)).astype(jnp.bfloat16)
    copies[1].wait()
    values = tok_ref[...].astype(jnp.float32)
    scale = lax.rsqrt(jnp.mean(values * values, axis=-1, keepdims=True) + NORM_EPS)
    copies[2].wait()
    normal = (values * scale * gain_ref[...]).astype(jnp.bfloat16)
    rows = dot(select, normal)
    own_ref[...] = rows[: wire.pad].astype(jnp.bfloat16)
    wire.pack(
        scratch,
        out_refs,
        lambda message, column: rows[wire.slot(message + 1), wire.block(column)],
    )


def arrange_kernel(*refs, wire):
    *wire_refs, x_ref, scratch = refs

    def put(message, column, rows):
        x_ref[wire.slot(message), wire.block(column)] = rows

    wire.unpack(wire_refs, scratch, put)


def unit(gate_pre, up_pre):
    gated = jnp.minimum(gate_pre, CLAMP_LIMIT)
    upper = jnp.clip(up_pre, -CLAMP_LIMIT, CLAMP_LIMIT)
    return ((upper + 1.0) * gated * jax.nn.sigmoid(SIGMOID_SCALE * gated)).astype(jnp.bfloat16)


def column_block(down_ref, group, core, width):
    if width % LANES == 0:
        start = (group * CORES + core) * width
        return down_ref[0, :, pl.ds(pl.multiple_of(start, width), width)]
    first, second = [
        down_ref[0, :, (group * CORES + i) * width : (group * CORES + i + 1) * width]
        for i in range(CORES)
    ]
    return jnp.where(core == 0, first, second)


def expert_kernel(*refs):
    *x_refs, gate_ref, up_ref, down_ref, hidden_ref, away_ref, x_ref = refs
    start = 0
    for ref in x_refs:
        x_ref[start : start + ref.shape[0]] = ref[...]
        start += ref.shape[0]
    hidden_ref[...] = unit(dot(x_ref[...], gate_ref[0]), dot(x_ref[...], up_ref[0]))
    other = (CORES - 1) - lax.axis_index("core")
    groups, _, width = away_ref.shape
    for group in range(groups):
        block = column_block(down_ref, group, other, width)
        away_ref[group] = dot(hidden_ref[...], block).astype(jnp.bfloat16)


def turned(eye, table):
    return lax.dot_general(
        eye, table, (((1,), (1,)), ((), ())), preferred_element_type=jnp.float32
    )


def third_kernel(hidden_ref, down_ref, route_ref, weight_ref, own_ref, mix_ref, *, wire):
    groups, _, width = own_ref.shape
    for group in range(groups):
        block = column_block(down_ref, group, lax.axis_index("core"), width)
        own_ref[group] = dot(hidden_ref[...], block)

    bf16, f32 = jnp.bfloat16, jnp.float32
    top_count, tok_count = route_ref.shape
    square = (tok_count, tok_count)
    down_at = lax.broadcasted_iota(jnp.int32, square, 0)
    across = lax.broadcasted_iota(jnp.int32, square, 1)
    eye = (down_at == across).astype(bf16)
    routes = turned(eye, route_ref[...].astype(bf16)).astype(jnp.int32)
    weights = weight_ref[...]
    high = weights.astype(bf16)
    low = (weights - high.astype(f32)).astype(bf16)
    weights = turned(eye, high) + turned(eye, low)
    lane = lax.broadcasted_iota(jnp.int32, (1, wire.rows), 1)
    message = lane // wire.stride
    offset = (lane - message * wire.stride).astype(f32)
    expert = message // groups
    weight = jnp.zeros((tok_count, wire.rows), f32)
    chosen = jnp.zeros((tok_count, wire.rows), f32)
    for k in range(top_count):
        at = routes[:, k : k + 1] == expert
        weight = jnp.where(at, weights[:, k : k + 1], weight)
        chosen = jnp.where(at, 1.0, chosen)
    rank = dot((across < down_at).astype(bf16), chosen.astype(bf16))
    away = offset - rank
    mix = jnp.concatenate(
        [
            jnp.where(away == float(column * wire.capacity), weight, 0.0)
            for column in range(wire.columns)
        ],
        axis=0,
    )
    high = mix.astype(bf16)
    mix_ref[0] = high
    mix_ref[1] = (mix - high.astype(f32)).astype(bf16)


def slot_of(block, core, rounds, count):
    step = step_from(lax.axis_index("ep"), block, count)
    slot = jnp.int32(0)
    for n, steps in enumerate(rounds):
        for at in range(CORES):
            if steps[at]:
                here = jnp.where(core == at, 1 + n, 1 + len(rounds) + n)
                slot = jnp.where(step == steps[at], here, slot)
    return slot


def add_kernel(own_ref, away_ref, out_ref, scratch, *, wire, rounds):
    groups = own_ref.shape[0]
    blocks = wire.messages // groups
    core = lax.axis_index("core")

    def starts(core):
        return [
            pl.multiple_of(slot_of(block, core, rounds, blocks) * wire.pad, wire.pad)
            for block in range(blocks)
        ]

    here, there = starts(core), starts((CORES - 1) - core)

    def get(message, column):
        block, group = divmod(message, groups)
        rows = pl.ds(here[block], wire.pad)
        theirs = pl.ds(there[block], wire.pad)
        lanes = wire.block(column)
        return own_ref[group, rows, lanes] + away_ref[group, theirs, lanes].astype(
            jnp.float32
        )

    wire.pack(scratch, [out_ref], get)


def combine_kernel(back_ref, mix_ref, out_ref, *, wire):
    tok_count = out_ref.shape[0]
    total = dot(mix_ref[0], back_ref[...]) + dot(mix_ref[1], back_ref[...])
    for column in range(wire.columns):
        rows = total[column * tok_count : (column + 1) * tok_count]
        out_ref[:, wire.block(column)] = rows.astype(jnp.bfloat16)


def in_hbm(array):
    return pltpu.with_memory_space_constraint(array, pltpu.HBM)


def call(kernel, out_shape, args, flops, moved, scratch=(), spaces=None, limit=16 * MIB):
    specs = spaces or [VMEM] * len(args)
    return pl.pallas_call(
        kernel,
        out_shape=out_shape,
        in_specs=specs,
        out_specs=jax.tree.map(lambda _: VMEM, out_shape),
        scratch_shapes=scratch,
        compiler_params=pltpu.CompilerParams(vmem_limit_bytes=limit),
        cost_estimate=pl.CostEstimate(flops=flops, bytes_accessed=moved, transcendentals=0),
    )(*args)


def local(tokens, norm_gain, routing, route_weight, w_gate, w_up, w_down):
    tok_count, width = tokens.shape
    top_count = routing.shape[1]
    blocks = lax.axis_size("ep")
    groups = lax.axis_size("y")
    experts = blocks * w_gate.shape[0]
    hidden_width = w_gate.shape[2]
    capacity = max(2, tok_count * top_count // experts + 1)
    half = width // CORES
    share = width // (groups * CORES)
    rounds = rounds_of(blocks)
    there = Wire(len(rounds), capacity, width)
    home = Wire(blocks * groups, capacity, share)
    rows = (1 + CORES * len(rounds)) * there.pad
    swap = [(i, CORES - 1 - i) for i in range(CORES)]
    routes = routing.T
    weights = route_weight.T
    bf16, f32 = jnp.bfloat16, jnp.float32
    shape = jax.ShapeDtypeStruct

    sending = call(
        functools.partial(gather_kernel, wire=there, rounds=rounds, count=blocks),
        (shape((there.pad, width), bf16),)
        + (shape((there.stride, there.lanes), bf16),) * len(rounds),
        [in_hbm(a) for a in (tokens, norm_gain.reshape(1, width), routes)],
        40 * 10**9,
        60 * 10**6,
        scratch=(
            pltpu.VMEM((tok_count, width), bf16),
            pltpu.VMEM((1, width), f32),
            pltpu.VMEM((top_count, tok_count), jnp.int32),
            there.scratch(),
            pltpu.SemaphoreType.DMA((3,)),
        ),
        spaces=[HBM, HBM, HBM],
    )
    came = []
    for steps, piece in zip(rounds, sending[1:]):
        pairs = [
            (place * CORES + at, joined(place, steps[at], blocks) * CORES + at)
            for place in range(blocks)
            for at in range(CORES)
        ]
        came.append(lax.ppermute(piece, ("ep", "core"), pairs))
    near, peer = [], []
    size = -(-len(rounds) // BATCHES)
    for start in range(0, len(rounds), size):
        batch = came[start : start + size]
        part = Wire(len(batch), capacity, width)
        near.append(
            call(
                functools.partial(arrange_kernel, wire=part),
                shape((len(batch) * part.pad, width), bf16),
                batch,
                len(batch) * part.pad * width,
                4 * len(batch) * part.pad * width,
                scratch=(part.scratch(),),
            )
        )
        peer.append(lax.ppermute(near[-1], "core", swap))
    step = 2 * rows * half * hidden_width
    hidden, away = call(
        expert_kernel,
        (shape((rows, hidden_width), bf16), shape((groups, rows, share), bf16)),
        (sending[0], *near, *peer, w_gate, w_up, w_down),
        5 * step,
        6 * width * hidden_width,
        scratch=(pltpu.VMEM((rows, width), bf16),),
    )
    arrived = lax.ppermute(away, "core", swap)
    kept, mix = call(
        functools.partial(third_kernel, wire=home),
        (
            shape((groups, rows, share), f32),
            shape((2, home.columns * tok_count, home.rows), bf16),
        ),
        (hidden, w_down, routes, weights),
        step,
        2 * half * hidden_width,
    )
    summed = call(
        functools.partial(add_kernel, wire=home, rounds=rounds),
        shape((home.rows, home.lanes), bf16),
        (kept, arrived),
        rows * half,
        8 * rows * half,
        scratch=(home.scratch(),),
    )
    back = lax.all_to_all(
        summed.reshape(blocks * groups, home.stride, home.lanes),
        ("ep", "y"),
        split_axis=0,
        concat_axis=0,
        tiled=True,
    ).reshape(home.rows, home.lanes)
    return call(
        functools.partial(combine_kernel, wire=home),
        shape((tok_count, share), bf16),
        (back, mix),
        4 * rows * tok_count * half,
        4 * rows * half,
    )


def solution(mesh):
    blocks, shares = mesh.devices.shape
    split = Mesh(mesh.devices.reshape(blocks, shares // CORES, CORES), ("ep", "y", "core"))
    tp = ("y", "core")
    placed = (
        P("ep", None),
        P(),
        P("ep", None),
        P("ep", None),
        P("ep", None, tp),
        P("ep", None, tp),
        P("ep", tp, None),
    )
    return jax.shard_map(
        local, mesh=split, in_specs=placed, out_specs=P("ep", tp), check_vma=False
    )
```
